32 devices in a mesh: ep: 8 (over z, y), tp: 4 (over x, core).
Axes of the slice: x: 2, y: 2, z: 4, core: 2. Of those that a mesh axis runs over, the one named last changes fastest.
Arguments:
- conv_value: bfloat16 [12288, 2048], P(('ep', 'tp')), may hold values from -6 to 6
- conv_gate: bfloat16 [12288, 2048], P(('ep', 'tp')), may hold values from -6 to 6
- conv_taps: float32 [31, 2048], replicated, may hold values from -1 to 1
- conv_gain: float32 [2048], replicated, may hold values from 0.1 to 1.9
- conv_bias: float32 [2048], replicated, may hold values from -3 to 3
- conv_projection: bfloat16 [2048, 4096], P(None, 'tp'), may hold values from -0.125 to 0.125
- expert_input: bfloat16 [4096, 4096], P('ep'), may hold values from -6 to 6
- expert_gain: float32 [4096], replicated, may hold values from 0.1 to 1.9
- route_experts: int32 [4096, 2], P('ep'), may hold values from 0 to 31, all different within a row; in each aligned block of 128 rows (0 to 127, 128 to 255, ...) at most 16 rows name the same one
- group_gate: float32 [4096], P('ep'), may hold values from 0.3 to 1
- expert_gate: float32 [4096, 2], P('ep'), may hold values from 0.1 to 1
- gate_weight: bfloat16 [32, 4096, 1024], P('ep', None, 'tp'), may hold values from -0.09375 to 0.09375
- up_weight: bfloat16 [32, 4096, 1024], P('ep', None, 'tp'), may hold values from -0.09375 to 0.09375
- down_weight: bfloat16 [32, 1024, 4096], P('ep', None, 'tp'), may hold values from -0.1875 to 0.1875
Outputs:
- conv_out: bfloat16 [12288, 4096], P('ep', 'tp')
- expert_out: bfloat16 [4096, 4096], P('ep', 'tp')
The draws below stay inside these ranges and needn't reach their ends.
Inputs may be any that keep to these rules, and one draw needn't show every extreme that they name: `route_experts`: each row names 2 different experts; in each aligned block of 128 rows no expert is named more than 16 times, and in some blocks one expert is named exactly 16 times.
All inputs are finite; a program needn't handle non-finite values.
Results may differ from the reference program's by a relative error of at most 0.0071.
Values may be sent and summed in bfloat16 or wider, within the bound.
A program may use at most 128 MiB of HBM per device.

```python
import math
import jax
import jax.numpy as jnp
import numpy as np
from jax import lax

D = 4096
CONV = 2048
KERNEL = 31
HID = 1024
EXPERTS = 32
TOP = 2
MOE_DEV = 128
CAP = 16
SEQ = 12288
MOE_ROWS = 4096


def level_of(stream_key, shape, split, low, largest):
    level = 1.0
    for position, blocks in split:
        draws = jax.random.uniform(jax.random.fold_in(jax.random.fold_in(stream_key, 6), position), (blocks,), jnp.float32, low / len(split), largest / len(split))
        level = level * jnp.repeat(jnp.exp(draws), shape[position] // blocks).reshape((-1,) + (1,) * (len(shape) - 1 - position))
    return level


def assign_block(stream_key, own, number, rows, number_of, top, limit, slope):
    sequence = jax.random.permutation(stream_key, number_of)
    crowded, common = portions_of(number_of, rows * top, limit, slope, True), portions_of(number_of, rows * top, limit, slope, False)
    places = jnp.arange(number_of)

    def named(tallies, offset_by):
        used = int((tallies > 0).sum())
        fixed = max(1, used // 4)
        passed = fixed + (places - fixed + offset_by * (used - fixed)) % max(1, number_of - fixed)
        return jnp.zeros((number_of,), jnp.int32).at[sequence[jnp.where(places < fixed, places, passed)]].set(jnp.asarray(tallies, jnp.int32))

    tallies = jnp.where(number % 4 == 0, named(crowded, number // 4), named(common, number - number // 4 - 1))
    mixed = jax.random.permutation(jax.random.fold_in(own, 3), number_of)
    donor, sink = mixed[0:number_of // 2 * 2:2], mixed[1:number_of // 2 * 2:2]
    margin = jnp.minimum(tallies[donor] - 1, limit - tallies[sink]) // 2
    margin = jnp.where((donor == sequence[0]) | (sink == sequence[0]) | (tallies[sink] == 0), 0, jnp.maximum(margin, 0))
    passed = jax.random.randint(jax.random.fold_in(own, 4), (number_of // 2,), 0, 1 << 20) % (margin + 1)
    tallies = tallies.at[donor].add(-passed).at[sink].add(passed)
    items = jnp.searchsorted(jnp.cumsum(tallies), jnp.arange(rows * top), side="right").astype(jnp.int32)
    table = items.reshape(top, rows).T
    table = table[jax.random.permutation(jax.random.fold_in(own, 1), rows)]
    offset_by = jax.random.randint(jax.random.fold_in(own, 2), (rows, 1), 0, top)
    return jnp.take_along_axis(table, (jnp.arange(top)[None, :] + offset_by) % top, axis=1)


def portions_of(count, total, bound, lean, full):
    weights = [(1 << 20) // math.isqrt(grade ** lean) + 1 for grade in range(1, count + 1)]
    largest = bound if full else min(bound, max(-(-total // count), total * weights[0] // sum(weights)))
    least = 1 if total - largest >= count - 1 else 0
    holding, rest = [largest] + [least] * (count - 1), total - largest - least * (count - 1)
    while rest > 0:
        candidates = [i for i in range(1, count) if holding[i] < largest] or [i for i in range(1, count) if holding[i] < bound]
        whole, remaining = sum([weights[i] for i in candidates]), rest
        for i in candidates:
            more = min(bound - holding[i], max(1, remaining * weights[i] // whole), rest)
            holding[i] = holding[i] + more
            rest = rest - more
    return np.array(holding)


def normal_values(rng, shape, deviation, most, shards=(), kind=jnp.bfloat16):
    level = level_of(rng, shape, shards, -0.22, 0.18) if shards else 1.0
    values = jax.random.normal(rng, shape, jnp.float32) * deviation * level
    return jnp.minimum(jnp.maximum(values, -most), most).astype(kind)


def setup_inputs(seed: int = 0) -> dict:
    splits = jax.random.split(jax.random.key(seed), 15)
    conv_value = normal_values(splits[0], (SEQ, CONV), 1.0, 6.0, ((0, 32),))
    conv_gate = normal_values(splits[1], (SEQ, CONV), 1.0, 6.0, ((0, 32),))
    conv_taps = normal_values(splits[2], (KERNEL, CONV), KERNEL ** -0.5, 1.0, (), jnp.float32)
    conv_gain = jnp.clip(1.0 + 0.18 * jax.random.normal(splits[3], (CONV,), jnp.float32), 0.1, 1.9)
    conv_bias = normal_values(splits[4], (CONV,), 0.5, 3.0, (), jnp.float32)
    conv_projection = normal_values(splits[5], (CONV, D), CONV ** -0.5, 0.125, ((1, 4),))
    expert_input = normal_values(splits[6], (MOE_ROWS, D), 1.0, 6.0, ((0, 8),))
    expert_gain = jnp.clip(1.0 + 0.18 * jax.random.normal(splits[7], (D,), jnp.float32), 0.1, 1.9)
    route_experts_keys = jax.random.split(jax.random.fold_in(splits[8], 1), MOE_ROWS // MOE_DEV)
    route_experts_turns = jax.random.permutation(jax.random.fold_in(splits[8], 3), MOE_ROWS // MOE_DEV)
    route_experts = jax.vmap(lambda own, number: assign_block(jax.random.fold_in(splits[8], 2), own, number, MOE_DEV, EXPERTS, TOP, CAP, 2))(route_experts_keys, route_experts_turns).reshape((MOE_ROWS, TOP))
    group_gate = jnp.clip(0.3 + 0.7 * jax.random.uniform(splits[9], (MOE_ROWS,), jnp.float32) ** level_of(splits[9], (MOE_ROWS,), ((0, 8),), -0.2, 0.2), 0.3, 1.0)
    expert_gate = jnp.clip(jnp.exp(math.log(1.0) - 2.3025851 * jax.random.uniform(splits[10], (MOE_ROWS, TOP), jnp.float32) ** level_of(splits[10], (MOE_ROWS, TOP), ((0, 8),), -0.2, 0.2)), 0.1, 1.0)
    gate_weight = normal_values(splits[11], (EXPERTS, D, HID), D ** -0.5, 0.09375, ((0, 8), (2, 4)))
    up_weight = normal_values(splits[12], (EXPERTS, D, HID), D ** -0.5, 0.09375, ((0, 8), (2, 4)))
    down_weight = normal_values(splits[13], (EXPERTS, HID, D), HID ** -0.5, 0.1875, ((0, 8), (2, 4)))
    return dict(conv_value=conv_value, conv_gate=conv_gate, conv_taps=conv_taps, conv_gain=conv_gain, conv_bias=conv_bias, conv_projection=conv_projection, expert_input=expert_input, expert_gain=expert_gain, route_experts=route_experts, group_gate=group_gate, expert_gate=expert_gate, gate_weight=gate_weight, up_weight=up_weight, down_weight=down_weight)


epsilon = 1e-06

def root_mean_norm(values, gain):
    widened = values.astype(jnp.float32)
    inverse_rms = lax.rsqrt(lax.optimization_barrier(jnp.mean(widened * widened, axis=-1, keepdims=True)) + epsilon)
    return (widened * inverse_rms * gain).astype(jnp.bfloat16)

def reference(conv_value, conv_gate, conv_taps, conv_gain, conv_bias, conv_projection, expert_input, expert_gain, route_experts, group_gate, expert_gate, gate_weight, up_weight, down_weight):
    gated_rows = (conv_value.astype(jnp.float32) * jax.nn.sigmoid(conv_gate.astype(jnp.float32))).astype(jnp.bfloat16)
    reach_back = KERNEL - 1
    extended = jnp.concatenate([jnp.zeros((reach_back, CONV), jnp.bfloat16), gated_rows], axis=0)
    mixed_conv = jnp.zeros((SEQ, CONV), jnp.float32)
    for lag_step in range(KERNEL):
        window = lax.slice_in_dim(extended, reach_back - lag_step, reach_back - lag_step + SEQ, axis=0)
        mixed_conv = mixed_conv + conv_taps[lag_step] * window.astype(jnp.float32)
    center = mixed_conv - lax.optimization_barrier(jnp.mean(mixed_conv, axis=-1, keepdims=True))
    spread = lax.optimization_barrier(jnp.mean(center * center, axis=-1, keepdims=True))
    activated = jax.nn.silu(center * lax.rsqrt(spread + epsilon) * conv_gain + conv_bias).astype(jnp.bfloat16)
    conv_out = jnp.dot(activated, conv_projection, preferred_element_type=jnp.float32).astype(jnp.bfloat16)
    normed = root_mean_norm(expert_input, expert_gain)
    blocks = MOE_ROWS // MOE_DEV
    picked_experts = route_experts.reshape(blocks, MOE_DEV * TOP)
    onehot = (picked_experts[:, :, None] == jnp.arange(EXPERTS, dtype=jnp.int32)[None, None, :]).astype(jnp.int32)
    before = jnp.cumsum(onehot, axis=1) - onehot
    positions = lax.optimization_barrier(jnp.sum(before * onehot, axis=2)).astype(jnp.int32)
    block_index = jnp.arange(blocks, dtype=jnp.int32)[:, None]
    token_index = block_index * MOE_DEV + jnp.arange(MOE_DEV * TOP, dtype=jnp.int32)[None, :] // TOP
    column = block_index * CAP + positions
    route_share = group_gate[:, None] * expert_gate / lax.optimization_barrier(jnp.sum(expert_gate, axis=1, keepdims=True))
    route_share = route_share.reshape(blocks, MOE_DEV * TOP)
    source = jnp.full((EXPERTS, blocks * CAP), -1, jnp.int32).at[picked_experts, column].set(token_index)
    shares = jnp.zeros((EXPERTS, blocks * CAP), jnp.float32).at[picked_experts, column].set(route_share)

    def one_expert(running, packed):
        indices, slot_shares, gate_matrix, up_matrix, down_matrix = packed
        safe_index = jnp.maximum(indices, 0)
        taken_rows = jnp.take(normed, safe_index, axis=0)
        gate_part = jnp.dot(taken_rows, gate_matrix, preferred_element_type=jnp.float32)
        up_part = jnp.dot(taken_rows, up_matrix, preferred_element_type=jnp.float32)
        hidden = (jax.nn.silu(gate_part) * up_part).astype(jnp.bfloat16)
        result = jnp.dot(hidden, down_matrix, preferred_element_type=jnp.float32).astype(jnp.bfloat16)
        return (running.at[safe_index].add(slot_shares[:, None] * result.astype(jnp.float32)), None)
    running, _ = lax.scan(one_expert, jnp.zeros((MOE_ROWS, D), jnp.float32), (source, shares, gate_weight, up_weight, down_weight))
    return (conv_out, running.astype(jnp.bfloat16))
```

```python
import functools

import jax
import jax.numpy as jnp
from jax import lax
from jax.experimental import pallas as pl
from jax.experimental.pallas import tpu as pltpu
from jax.sharding import PartitionSpec as P

EXPERTS = 32
TOP = 2
MOE_DEV = 128
CAP = 16

MESH = pl.DeviceIdType.MESH

epsilon = 1e-06


def passed_along(value, axis, steps):
    count = lax.axis_size(axis)
    leading, last = (max(0, -steps), min(count, count - steps))
    return lax.ppermute(value, axis, [(source, source + steps) for source in range(leading, last)])


def root_mean_norm(values, gain):
    widened = values.astype(jnp.float32)
    inverse_rms = lax.rsqrt(jnp.mean(widened * widened, axis=-1, keepdims=True) + epsilon)
    return (widened * inverse_rms * gain).astype(jnp.bfloat16)


def slot_numbers(route_experts):
    picked = route_experts.reshape(-1, MOE_DEV * TOP)
    onehot = (picked[:, :, None] == jnp.arange(EXPERTS, dtype=jnp.int32)).astype(jnp.bfloat16)
    order = jnp.arange(MOE_DEV * TOP, dtype=jnp.int32)
    earlier = (order[:, None] > order[None, :]).astype(jnp.bfloat16)
    before = jnp.einsum("ij,bje->bie", earlier, onehot, preferred_element_type=jnp.float32)
    positions = jnp.sum(before * onehot.astype(jnp.float32), axis=2).astype(jnp.int32)
    return (picked * CAP + positions).reshape(-1, MOE_DEV, TOP)


def stepped(move):
    ring = move // 2
    return (ring + 1) // 2 * (2 * (ring % 2) - 1), move % 2


def moved(source, move, count):
    along, across = stepped(move)
    rings = count // 2
    return (source // 2 + along + rings) % rings * 2 + (source % 2 + across) % 2


def came_from(target, move, count):
    along, across = stepped(move)
    rings = count // 2
    return (target // 2 - along + rings) % rings * 2 + (target % 2 + across) % 2


def slots_filled(normed, slots, wanted):
    chosen = jnp.any(slots[:, None, :, :] == wanted[None, :, None, None], axis=3)
    return jnp.einsum(
        "qsr,qrd->qsd", chosen.astype(jnp.bfloat16), normed, preferred_element_type=jnp.float32
    ).astype(jnp.bfloat16)


def expert_kernel(
    count,
    lag,
    chunks,
    home,
    gate_hbm,
    up_hbm,
    down_hbm,
    returned,
    landed,
    gate,
    up,
    down,
    hidden,
    result,
    load_sem,
    first_send,
    first_recv,
    side_send,
    side_recv,
    near_send,
    near_recv,
    unit_send,
    unit_recv,
    back_send,
    back_recv,
):
    group, quarter = lax.axis_index("ep"), lax.axis_index("tp")
    near, side = quarter + 1 - 2 * (quarter % 2), (quarter + 2) % 4
    local = gate.shape[0]

    loads = [
        pltpu.make_async_copy(source, target, load_sem.at[number])
        for number, (source, target) in enumerate(
            [(home, landed.at[0]), (gate_hbm, gate), (up_hbm, up), (down_hbm, down)]
        )
    ]
    for load in loads:
        load.start()

    barrier = pltpu.get_barrier_semaphore()

    def greet(m, carry):
        pl.semaphore_signal(
            barrier, inc=1, device_id=(moved(group, m, count), quarter), device_id_type=MESH
        )
        return carry

    lax.fori_loop(1, count, greet, 0)
    for other in (near, side):
        pl.semaphore_signal(barrier, inc=1, device_id=(group, other), device_id_type=MESH)
    pl.semaphore_wait(barrier, count + 1)

    def copy(source, target, send, recv, device):
        return pltpu.make_async_remote_copy(
            src_ref=source,
            dst_ref=target,
            send_sem=send,
            recv_sem=recv,
            device_id=device,
            device_id_type=MESH,
        )

    def first(m):
        place = landed.at[m, quarter]
        device = (moved(group, m, count), quarter)
        return copy(chunks.at[m - 1], place, first_send.at[m], first_recv.at[m], device)

    def to_side(m):
        place = landed.at[m, quarter]
        return copy(place, place, side_send.at[m], side_recv.at[m], (group, side))

    def to_near(m, number):
        place = landed.at[m, (quarter, side)[number]]
        send, recv = near_send.at[m, number], near_recv.at[m, number]
        return copy(place, place, send, recv, (group, near))

    def units(p, number):
        place = hidden.at[p, (quarter, quarter, side)[number]]
        send, recv = unit_send.at[p, number], unit_recv.at[p, number]
        return copy(place, place, send, recv, (group, (side, near, near)[number]))

    def back(m):
        device = (came_from(group, m, count), quarter)
        return copy(result.at[m], returned.at[m], back_send.at[m], back_recv.at[m], device)

    def kept():
        return pltpu.make_async_copy(result.at[0], returned.at[0], load_sem.at[4])

    def start_first(m, carry):
        first(m).start()
        return carry

    lax.fori_loop(1, count, start_first, 0)

    def to_hidden(p):
        for e in range(local):
            rows = landed[p, :, e * CAP : (e + 1) * CAP, :]
            rows = rows.reshape(rows.shape[0] * CAP, rows.shape[2])
            gate_part = jnp.dot(rows, gate[e], preferred_element_type=jnp.float32)
            up_part = jnp.dot(rows, up[e], preferred_element_type=jnp.float32)
            part = (gate_part / (1.0 + jnp.exp(-gate_part)) * up_part).astype(jnp.bfloat16)
            part = part.reshape(-1, CAP, part.shape[1])
            hidden[p, quarter, :, e * CAP : (e + 1) * CAP, :] = part

    def to_result(p):
        for e in range(local):
            parts = [hidden[p, t, :, e * CAP : (e + 1) * CAP, :] for t in range(hidden.shape[1])]
            parts = [part.reshape(-1, part.shape[2]) for part in parts]
            total = jnp.dot(
                jnp.concatenate(parts, axis=1), down[e], preferred_element_type=jnp.float32
            )
            total = total.astype(jnp.bfloat16).reshape(-1, CAP, total.shape[1])
            result[p, :, e * CAP : (e + 1) * CAP, :] = total

    loads[0].wait()
    loads[1].wait()
    loads[2].wait()

    def step(j, carry):
        @pl.when((j >= 1) & (j < count))
        def _():
            first(j).wait_recv()
            to_side(j).start()
            to_near(j, 0).start()

        @pl.when((j >= 2) & (j < count + 1))
        def _():
            to_side(j - 1).wait_recv()
            to_near(j - 1, 1).start()

        @pl.when((j >= 3) & (j < count + 2))
        def _():
            to_near(j - 2, 0).wait_recv()
            to_near(j - 2, 1).wait_recv()

        @pl.when((j >= 3) & (j < count + 3))
        def _():
            units(j - 3, 0).start()
            units(j - 3, 1).start()

        @pl.when((j >= 2) & (j < count + 2))
        def _():
            to_hidden(j - 2)

        late = j - 3 - lag

        @pl.when((late >= 2) & (late < count + 2))
        def _():
            @pl.when(late == 2)
            def _():
                kept().start()

            @pl.when(late > 2)
            def _():
                back(late - 2).start()

        @pl.when((late >= 0) & (late < count))
        def _():
            units(late, 0).wait_recv()
            units(late, 2).start()

        @pl.when((late >= 1) & (late < count + 1))
        def _():
            @pl.when(late == 1)
            def _():
                loads[3].wait()

            units(late - 1, 1).wait_recv()
            units(late - 1, 2).wait_recv()
            to_result(late - 1)

        return carry

    lax.fori_loop(1, count + 5 + lag, step, 0)

    def finish(m, carry):
        first(m).wait_send()
        to_side(m).wait_send()
        to_near(m, 0).wait_send()
        to_near(m, 1).wait_send()
        back(m).wait()
        return carry

    lax.fori_loop(1, count, finish, 0)

    def finish_units(p, carry):
        for number in range(3):
            units(p, number).wait_send()
        return carry

    lax.fori_loop(0, count, finish_units, 0)
    kept().wait()


def by_experts(chunks, home, gate_weight, up_weight, down_weight, count):
    quarters, size, width = home.shape
    units, features = gate_weight.shape[2], down_weight.shape[2]
    rows = count * quarters * size
    dma = pltpu.SemaphoreType.DMA
    return pl.pallas_call(
        functools.partial(expert_kernel, count, 1),
        out_shape=jax.ShapeDtypeStruct((count, quarters, size, features), jnp.bfloat16),
        in_specs=[pl.BlockSpec(memory_space=pl.ANY)] * 5,
        out_specs=pl.BlockSpec(memory_space=pl.ANY),
        scratch_shapes=[
            pltpu.VMEM((count, quarters, size, width), jnp.bfloat16),
            pltpu.VMEM(gate_weight.shape, jnp.bfloat16),
            pltpu.VMEM(up_weight.shape, jnp.bfloat16),
            pltpu.VMEM(down_weight.shape, jnp.bfloat16),
            pltpu.VMEM((count, quarters, quarters, size, units), jnp.bfloat16),
            pltpu.VMEM((count, quarters, size, features), jnp.bfloat16),
            dma((5,)),
            dma((count,)),
            dma((count,)),
            dma((count,)),
            dma((count,)),
            dma((count, 2)),
            dma((count, 2)),
            dma((count, 3)),
            dma((count, 3)),
            dma((count,)),
            dma((count,)),
        ],
        compiler_params=pltpu.CompilerParams(
            collective_id=0, has_side_effects=True, vmem_limit_bytes=58 * 1024 * 1024
        ),
        cost_estimate=pl.CostEstimate(
            flops=40 * rows * width * units, bytes_accessed=250_000_000, transcendentals=0
        ),
    )(chunks, home, gate_weight, up_weight, down_weight)


def weighed(results, slots, share, wanted):
    same = slots[:, :, :, None] == wanted[None, None, None, :]
    weights = jnp.sum(jnp.where(same, share[:, :, :, None], 0.0), axis=2)
    high = weights.astype(jnp.bfloat16)
    low = (weights - high.astype(jnp.float32)).astype(jnp.bfloat16)
    both = jnp.concatenate([high, low], axis=1)
    both = both.reshape(both.shape[:2] + (results.shape[0], results.shape[2]))
    total = jnp.einsum("qrks,kqsd->qrd", both, results, preferred_element_type=jnp.float32)
    return total[:, : total.shape[1] // 2] + total[:, total.shape[1] // 2 :]


def convolved(conv_value, conv_gate, conv_taps, conv_gain, conv_bias):
    gated_rows = (
        conv_value.astype(jnp.float32) * jax.nn.sigmoid(conv_gate.astype(jnp.float32))
    ).astype(jnp.bfloat16)
    reach_back = conv_taps.shape[0] - 1
    length = gated_rows.shape[0]
    earlier = passed_along(gated_rows[length - reach_back :], ("ep", "tp"), 1)
    extended = jnp.concatenate([earlier, gated_rows], axis=0)
    mixed_conv = jnp.zeros(gated_rows.shape, jnp.float32)
    for lag_step in range(reach_back + 1):
        window = lax.slice_in_dim(
            extended, reach_back - lag_step, reach_back - lag_step + length, axis=0
        )
        mixed_conv = mixed_conv + conv_taps[lag_step] * window.astype(jnp.float32)
    center = mixed_conv - jnp.mean(mixed_conv, axis=-1, keepdims=True)
    spread = jnp.mean(center * center, axis=-1, keepdims=True)
    return jax.nn.silu(center * lax.rsqrt(spread + epsilon) * conv_gain + conv_bias).astype(
        jnp.bfloat16
    )


def on_device(
    conv_value,
    conv_gate,
    conv_taps,
    conv_gain,
    conv_bias,
    conv_projection,
    expert_input,
    expert_gain,
    route_experts,
    group_gate,
    expert_gate,
    gate_weight,
    up_weight,
    down_weight,
):
    count = lax.axis_size("ep")
    own_group = lax.axis_index("ep")
    own_quarter = lax.axis_index("tp")
    local = gate_weight.shape[0]
    size = local * CAP
    slots = slot_numbers(route_experts)
    quarters = slots.shape[0]
    share = group_gate[:, None] * expert_gate / jnp.sum(expert_gate, axis=1, keepdims=True)
    share = share.reshape(slots.shape)
    own_rows = lax.dynamic_slice_in_dim(expert_input, own_quarter * MOE_DEV, MOE_DEV, 0)
    own_normed = root_mean_norm(own_rows, expert_gain)[None]
    own_slots = lax.dynamic_slice_in_dim(slots, own_quarter, 1, 0)

    activated = convolved(conv_value, conv_gate, conv_taps, conv_gain, conv_bias)
    firsts = jnp.stack([moved(own_group, move, count) for move in range(count)]) * size
    wanted = (firsts[:, None] + jnp.arange(size, dtype=jnp.int32)).reshape(-1)
    chunks = slots_filled(own_normed, own_slots, wanted[size:])[0].reshape(count - 1, size, -1)
    normed = root_mean_norm(expert_input, expert_gain).reshape(quarters, MOE_DEV, -1)
    home = slots_filled(normed, slots, wanted[:size])
    chunks, activated = lax.optimization_barrier((chunks, activated))
    results = by_experts(chunks, home, gate_weight, up_weight, down_weight, count)
    total = weighed(results, slots, share, wanted)
    expert_out = total.reshape(quarters * MOE_DEV, -1).astype(jnp.bfloat16)
    conv_out = jnp.dot(
        lax.all_gather(activated, "tp", axis=0, tiled=True),
        conv_projection,
        preferred_element_type=jnp.float32,
    ).astype(jnp.bfloat16)
    return (conv_out, expert_out)


def solution(mesh):
    return jax.shard_map(
        on_device,
        mesh=mesh,
        in_specs=(
            P(("ep", "tp"), None),
            P(("ep", "tp"), None),
            P(),
            P(),
            P(),
            P(None, "tp"),
            P("ep", None),
            P(),
            P("ep", None),
            P("ep"),
            P("ep", None),
            P("ep", None, "tp"),
            P("ep", None, "tp"),
            P("ep", None, "tp"),
        ),
        out_specs=(P("ep", "tp"), P("ep", "tp")),
        check_vma=False,
    )
```
